32 devices in a mesh: dp: 2 (over y), kv: 16 (over z, x, core), tp: 1.
Axes of the slice: x: 2, y: 2, z: 4, core: 2. Of those that a mesh axis runs over, the one named last changes fastest.
Arguments:
- tokens: bfloat16 [16, 4096], P('dp', 'kv'), may hold values from -6 to 6
- attn_gain: float32 [4096], P('kv'), may hold values from 0.1 to 1.9
- query_weight: bfloat16 [4096, 2048], P('kv', 'tp'), may hold values from -0.09375 to 0.09375
- key_cache: bfloat16 [16, 2048, 8, 2, 128], P('dp', 'kv', 'tp'), may hold values from -1024 to 1024
- value_cache: bfloat16 [16, 2048, 8, 256], P('dp', 'kv', 'tp'), may hold values from -6 to 6
- lambdas: float32 [8], P('tp'), may hold values from 0.3 to 0.8
- head_gain: float32 [256], replicated, may hold values from 0.1 to 1.9
- out_weight: bfloat16 [2048, 4096], P('tp', 'kv'), may hold values from -0.125 to 0.125
- mixer_gain: float32 [4096], P('kv'), may hold values from 0.1 to 1.9
- up_weight: bfloat16 [4096, 16384], P('kv', 'tp'), may hold values from -0.09375 to 0.09375
- down_weight: bfloat16 [16384, 4096], P('tp', 'kv'), may hold values from -0.046875 to 0.046875
Outputs:
- result: bfloat16 [16, 4096], P('dp', 'kv')
The draws below stay inside these ranges and needn't reach their ends.
All inputs are finite; a program needn't handle non-finite values.
Results may differ from the reference program's by a relative error of at most 0.024.
Values may be sent and summed in bfloat16 or wider, within the bound.
A program may use at most 64 MiB of HBM per device.

```python
import math
import jax
import jax.numpy as jnp
from jax import lax

D = 4096
HEADS = 8
HEAD = 128
VDIM = 256
FF = 16384
BATCH = 16
LEN = 2048


def draw_tokens(key, part):
    first = jax.random.fold_in(key, 0)
    column = jnp.arange(D, dtype=jnp.float32) / D
    noise = jnp.clip(jax.random.normal(first, (BATCH, D), jnp.float32), -6.0, 6.0)
    scale = 0.3 * (1.0 + 2.0 * column)
    return (noise * scale).astype(jnp.bfloat16)


def draw_key_cache(key, part):
    parts_keys = jax.random.split(key, 1)
    base = 1.75 * jnp.clip(jax.random.normal(parts_keys[0], (BATCH, LEN, HEADS, 2, HEAD), jnp.float32), -6.0, 6.0)
    return base.astype(jnp.bfloat16)


def block_scale(key, shape, cuts, low, high):
    def one(dim, blocks):
        heights = jax.random.uniform(jax.random.fold_in(jax.random.fold_in(key, 6), dim), (blocks,), jnp.float32, low / len(cuts), high / len(cuts))
        return jnp.repeat(jnp.exp(heights), shape[dim] // blocks).reshape((-1,) + (1,) * (len(shape) - dim - 1))

    loudness = one(*cuts[0])
    for cut in cuts[1:]:
        loudness = loudness * one(*cut)
    return loudness


def normal_values(own_key, dims, deviation, most, cuts=(), held_as=jnp.bfloat16):
    values = deviation * jax.random.normal(own_key, dims, jnp.float32)
    if cuts:
        values = values * block_scale(own_key, dims, cuts, -0.22, 0.18)
    return jnp.clip(values, -most, most).astype(held_as)


def setup_inputs(seed: int = 0) -> dict:
    splits = jax.random.split(jax.random.key(seed), 12)
    return {
        "tokens": draw_tokens(jax.random.fold_in(splits[11], 71), 0),
        "attn_gain": jnp.clip(1.0 + 0.18 * jax.random.normal(splits[1], (D,), jnp.float32), 0.1, 1.9),
        "query_weight": normal_values(splits[2], (D, HEADS * 2 * HEAD), D ** -0.5, 0.09375, ((0, 16),)),
        "key_cache": draw_key_cache(jax.random.fold_in(splits[11], 71), 0),
        "value_cache": normal_values(splits[4], (BATCH, LEN, HEADS, VDIM), 1.0, 6.0, ((0, 2), (1, 16))),
        "lambdas": jnp.clip(jax.random.uniform(splits[5], (HEADS,), jnp.float32, 0.3, 0.8), 0.3, 0.8),
        "head_gain": jnp.clip(1.0 + 0.18 * jax.random.normal(splits[6], (VDIM,), jnp.float32), 0.1, 1.9),
        "out_weight": normal_values(splits[7], (HEADS * VDIM, D), (HEADS * VDIM) ** -0.5, 0.125, ((1, 16),)),
        "mixer_gain": jnp.clip(1.0 + 0.18 * jax.random.normal(splits[8], (D,), jnp.float32), 0.1, 1.9),
        "up_weight": normal_values(splits[9], (D, FF), D ** -0.5, 0.09375, ((0, 16),)),
        "down_weight": normal_values(splits[10], (FF, D), FF ** -0.5, 0.046875, ((1, 16),)),
    }


EPS = 1e-05

def rotate(query, position):
    half = query.shape[-1] // 2
    inverse = 10000.0 ** (-jnp.arange(half, dtype=jnp.float32) / half)
    angle = jnp.float32(position) * inverse
    cosine = jnp.cos(angle)
    sine = jnp.sin(angle)
    first = query[..., :half]
    second = query[..., half:]
    return jnp.concatenate([first * cosine - second * sine, second * cosine + first * sine], axis=-1)

def attend_one(item):
    query, keys, values = item
    scores = jnp.einsum('hcd,khcd->hck', query.astype(jnp.float32), keys.astype(jnp.float32)) / math.sqrt(HEAD)
    top = lax.optimization_barrier(jnp.max(scores, axis=-1, keepdims=True))
    expo = jnp.exp(scores - top)
    denom = lax.optimization_barrier(jnp.sum(expo, axis=-1))
    expo_b = lax.optimization_barrier(expo.astype(jnp.bfloat16)).astype(jnp.float32)
    numer = jnp.einsum('hck,khv->hcv', expo_b, values.astype(jnp.float32))
    return numer / denom[..., None]

def reference(tokens, attn_gain, query_weight, key_cache, value_cache, lambdas, head_gain, out_weight, mixer_gain, up_weight, down_weight):
    tok_float = tokens.astype(jnp.float32)
    attn_inv = lax.rsqrt(lax.optimization_barrier(jnp.sum(tok_float * tok_float, axis=1)) / D + EPS)
    scaled_in = (tok_float * attn_gain).astype(jnp.bfloat16)
    query_raw = jnp.dot(scaled_in, query_weight, preferred_element_type=jnp.float32)
    query = rotate((attn_inv[:, None] * query_raw).reshape(BATCH, HEADS, 2, HEAD), LEN - 1).astype(jnp.bfloat16)
    ratio = lax.map(attend_one, (query, key_cache, value_cache))
    mixed = ratio[:, :, 0] - lambdas[None, :, None] * ratio[:, :, 1]
    normed = mixed * lax.rsqrt(lax.optimization_barrier(jnp.mean(mixed * mixed, axis=-1, keepdims=True)) + EPS) * head_gain
    normed = normed.astype(jnp.bfloat16).reshape(BATCH, HEADS * VDIM)
    attn_out = jnp.dot(normed, out_weight, preferred_element_type=jnp.float32)
    middle = (tok_float + attn_out).astype(jnp.bfloat16)
    mid_float = middle.astype(jnp.float32)
    mixer_inv = lax.rsqrt(lax.optimization_barrier(jnp.sum(mid_float * mid_float, axis=1)) / D + EPS)
    mixer_in = (mid_float * mixer_gain).astype(jnp.bfloat16)
    up_raw = jnp.dot(mixer_in, up_weight, preferred_element_type=jnp.float32)
    hidden = jnp.square(jax.nn.relu(mixer_inv[:, None] * up_raw)).astype(jnp.bfloat16)
    mixer_out = jnp.dot(hidden, down_weight, preferred_element_type=jnp.float32)
    return (mid_float + mixer_out).astype(jnp.bfloat16)
```

```python
import functools
import math

import jax
import jax.numpy as jnp
import numpy as np
from jax import lax
from jax.experimental import pallas as pl
from jax.experimental.pallas import tpu as pltpu
from jax.sharding import PartitionSpec as P

EPS = 1e-05
F32 = jnp.float32
BF16 = jnp.bfloat16


def merged(value, axis, combine):
    everything = jax.tree.map(lambda part: lax.all_gather(part, axis), value)
    initial = jax.tree.map(lambda part: part[0], everything)

    def lap(k, so_far):
        return combine(so_far, jax.tree.map(lambda part: part[k], everything))

    return lax.fori_loop(1, lax.axis_size(axis), lap, initial)


def rotate(query, position):
    half = query.shape[-1] // 2
    inverse = 10000.0 ** (-jnp.arange(half, dtype=jnp.float32) / half)
    angle = jnp.float32(position) * inverse
    cosine = jnp.cos(angle)
    sine = jnp.sin(angle)
    first = query[..., :half]
    second = query[..., half:]
    return jnp.concatenate(
        [first * cosine - second * sine, second * cosine + first * sine], axis=-1
    )


def combine_partial(earlier, later):
    top_a, total_a, numer_a = earlier
    top_b, total_b, numer_b = later
    top = jnp.maximum(top_a, top_b)
    factor_a = jnp.exp(top_a - top)
    factor_b = jnp.exp(top_b - top)
    return (
        top,
        total_a * factor_a + total_b * factor_b,
        numer_a * factor_a[..., None] + numer_b * factor_b[..., None],
    )


def local(
    tokens,
    attn_gain,
    query_weight,
    key_cache,
    value_cache,
    lambdas,
    head_gain,
    out_weight,
    mixer_gain,
    up_weight,
    down_weight,
):
    row_count = tokens.shape[0]
    width = tokens.shape[1] * lax.axis_size("kv")
    local_heads = key_cache.shape[2]
    head_width = key_cache.shape[4]
    length = key_cache.shape[1] * lax.axis_size("kv")
    tok_float = tokens.astype(jnp.float32)
    own_squares = jnp.sum(tok_float * tok_float, axis=1)
    scaled_in = (tok_float * attn_gain).astype(jnp.bfloat16)
    query_part = jnp.dot(scaled_in, query_weight, preferred_element_type=jnp.float32)
    squares = lax.psum(own_squares, "kv")
    query_raw = lax.psum(query_part, "kv")
    attn_inv = lax.rsqrt(squares / width + EPS)
    shaped = (attn_inv[:, None] * query_raw).reshape(row_count, local_heads, 2, head_width)
    query = rotate(shaped, length - 1).astype(jnp.bfloat16)
    scores = jnp.einsum(
        "bhcd,bkhcd->bhck", query, key_cache, preferred_element_type=jnp.float32
    ) / math.sqrt(head_width)
    top = jnp.max(scores, axis=-1)
    expo = jnp.exp(scores - top[..., None])
    denom = jnp.sum(expo, axis=-1)
    numer = jnp.einsum(
        "bhck,bkhv->bhcv",
        expo.astype(jnp.bfloat16),
        value_cache,
        preferred_element_type=jnp.float32,
    )
    top, denom, numer = merged((top, denom, numer), "kv", combine_partial)
    ratio = numer / denom[..., None]
    mixed = ratio[:, :, 0] - lambdas[None, :, None] * ratio[:, :, 1]
    normed = mixed * lax.rsqrt(jnp.mean(mixed * mixed, axis=-1, keepdims=True) + EPS) * head_gain
    normed = normed.astype(jnp.bfloat16).reshape(row_count, -1)
    attn_part = jnp.dot(normed, out_weight, preferred_element_type=jnp.float32)
    attn_out = lax.psum(attn_part, "tp")
    middle = (tok_float + attn_out).astype(jnp.bfloat16)
    mid_float = middle.astype(jnp.float32)
    mix_squares = lax.psum(jnp.sum(mid_float * mid_float, axis=1), "kv")
    mixer_inv = lax.rsqrt(mix_squares / width + EPS)
    mixer_in = (mid_float * mixer_gain).astype(jnp.bfloat16)
    up_part = jnp.dot(mixer_in, up_weight, preferred_element_type=jnp.float32)
    share = lax.psum_scatter(up_part, "kv", scatter_dimension=1, tiled=True)
    hidden_share = jnp.square(jax.nn.relu(mixer_inv[:, None] * share)).astype(jnp.bfloat16)
    mixer_part = jnp.dot(
        lax.all_gather(hidden_share, "kv", axis=1, tiled=True),
        down_weight,
        preferred_element_type=jnp.float32,
    )
    mixer_out = lax.psum(mixer_part, "tp")
    return (mid_float + mixer_out).astype(jnp.bfloat16)


def layer_kernel(
    n,
    width,
    tok_ref,
    again_ref,
    lam_ref,
    hgain_ref,
    mgain_ref,
    cos_ref,
    sin_ref,
    wq_hbm,
    k_hbm,
    v_hbm,
    wo_hbm,
    wu_hbm,
    wd_hbm,
    out_ref,
    wq,
    kc,
    vc,
    wo,
    wu,
    wd,
    q_send,
    q_recv,
    q_all,
    a_send,
    a_recv,
    n_all,
    u_send,
    u_recv,
    h_all,
    load_sem,
    send_sem,
    recv_sem,
):
    rows, feats = tok_ref.shape
    hd = cos_ref.shape[1]
    maps = wq.shape[1] // hd
    heads = maps // 2
    vdim = vc.shape[2]
    share = wu.shape[1] // n
    per = maps * rows // n
    me = lax.axis_index("kv")

    loads = [
        pltpu.make_async_copy(src, dst, load_sem.at[i])
        for i, (src, dst) in enumerate(
            [(wq_hbm, wq), (k_hbm, kc), (v_hbm, vc), (wo_hbm, wo), (wu_hbm, wu), (wd_hbm, wd)]
        )
    ]
    loads[0].start()
    loads[1].start()

    barrier = pltpu.get_barrier_semaphore()

    def greet(k, carry):
        pl.semaphore_signal(barrier, inc=1, device_id={"kv": lax.rem(me + k, n)})
        return carry

    lax.fori_loop(1, n, greet, 0)

    def to_peer(phase, k, src, dst):
        return pltpu.make_async_remote_copy(
            src_ref=src,
            dst_ref=dst,
            send_sem=send_sem.at[phase, k],
            recv_sem=recv_sem.at[phase, k],
            device_id={"kv": lax.rem(me + k, n)},
        )

    def over_peers(body):
        lax.fori_loop(1, n, lambda k, c: (body(k), c)[1], 0)

    tok = tok_ref[...].astype(F32)
    squares = jnp.sum(tok * tok, axis=1, keepdims=True)
    scaled = (tok * again_ref[...]).astype(BF16)
    loads[0].wait()
    for load in loads[2:]:
        load.start()
    query = jnp.dot(scaled, wq[...], preferred_element_type=F32)
    for m in range(n):
        q_send[m, :, :hd] = query[:, m * hd : (m + 1) * hd]
        q_send[m, :, hd:] = jnp.broadcast_to(squares, (rows, hd))
    pl.semaphore_wait(barrier, n - 1)
    over_peers(
        lambda k: to_peer(0, k, q_send.at[lax.rem(me + k, n)], q_recv.at[k]).start()
    )
    total = q_send[me]
    for k in range(1, n):
        to_peer(0, k, q_send.at[0], q_recv.at[k]).wait_recv()
        total += q_recv[k]
    inv = lax.rsqrt(total[:, hd:] / width + EPS)
    raw = inv * total[:, :hd]
    turned = raw * cos_ref[...] + pltpu.roll(raw, hd // 2, 1) * sin_ref[...]
    q_all[me] = turned.astype(BF16)
    over_peers(lambda k: to_peer(1, k, q_all.at[me], q_all.at[me]).start())
    over_peers(
        lambda k: to_peer(
            1, k, q_all.at[me], q_all.at[lax.rem(me + n - k, n)]
        ).wait_recv()
    )

    q_float = q_all[...].astype(F32)
    q_rows = jnp.swapaxes(q_float, 0, 1)
    loads[1].wait()
    loads[2].wait()
    lanes = kc.shape[1]
    own_map = lax.broadcasted_iota(jnp.int32, (maps, lanes), 0) == (
        lax.broadcasted_iota(jnp.int32, (maps, lanes), 1) % maps
    )
    fold = (
        lax.broadcasted_iota(jnp.int32, (256, 128), 0) // 2
        == lax.broadcasted_iota(jnp.int32, (256, 128), 1)
    ).astype(F32).astype(BF16)
    lane = lax.broadcasted_iota(jnp.int32, (maps, 128), 1)
    for b in range(rows):
        scores = lax.dot_general(
            q_rows[b].astype(BF16),
            kc[b],
            (((1,), (1,)), ((), ())),
            preferred_element_type=F32,
        ) * (1.0 / math.sqrt(hd))
        scores = jnp.where(own_map, scores, -jnp.inf)
        top = jnp.max(scores, axis=1, keepdims=True)
        expo = jnp.exp(scores - top)
        denom = jnp.sum(expo, axis=1, keepdims=True)
        expo_b = expo.astype(BF16)
        folded = jnp.concatenate(
            [
                jnp.dot(expo_b[:, i : i + 256], fold, preferred_element_type=F32)
                for i in range(0, lanes, 256)
            ],
            axis=1,
        ).astype(BF16)
        numer = jnp.dot(folded, vc[b], preferred_element_type=F32)
        stats = jnp.where(lane < 64, top, denom)
        step = maps // per
        for part in range(step):
            slot = b * step + part
            a_send[slot, :, :vdim] = numer[part * per : (part + 1) * per]
            a_send[slot, :, vdim:] = stats[part * per : (part + 1) * per]
    over_peers(
        lambda k: to_peer(2, k, a_send.at[lax.rem(me + k, n)], a_recv.at[k]).start()
    )
    a_recv[0] = a_send[me]
    for k in range(1, n):
        to_peer(2, k, a_send.at[0], a_recv.at[k]).wait_recv()
    tops = [a_recv[k, :, vdim : vdim + 1] for k in range(n)]
    top = functools.reduce(jnp.maximum, tops)
    numer = jnp.zeros((per, vdim), F32)
    denom = jnp.zeros((per, 1), F32)
    for k in range(n):
        factor = jnp.exp(tops[k] - top)
        numer += factor * a_recv[k, :, :vdim]
        denom += factor * a_recv[k, :, vdim + 64 : vdim + 65]
    ratio = numer / denom
    row = lax.broadcasted_iota(jnp.int32, (per, 1), 0)
    first_head = lax.rem(me, maps // per) * (per // 2)
    sign = jnp.ones((per, 1), F32)
    for h in range(per // 2):
        sign = jnp.where(row == 2 * h + 1, -lam_ref[first_head + h], sign)
    signed = ratio * sign
    mixed = signed + pltpu.roll(signed, per - 1, 0)
    normed = (
        mixed
        * lax.rsqrt(jnp.sum(mixed * mixed, axis=1, keepdims=True) / vdim + EPS)
        * hgain_ref[...]
    )
    n_all[me] = normed.astype(BF16)
    over_peers(lambda k: to_peer(3, k, n_all.at[me], n_all.at[me]).start())
    over_peers(
        lambda k: to_peer(
            3, k, n_all.at[me], n_all.at[lax.rem(me + n - k, n)]
        ).wait_recv()
    )

    stacked = n_all[...].astype(F32).reshape(rows * maps, vdim)
    which = lax.broadcasted_iota(jnp.int32, (rows * maps, vdim), 0) % maps
    loads[3].wait()
    spread = jnp.zeros((rows * maps, feats), F32)
    for h in range(heads):
        spread += jnp.dot(
            jnp.where(which == 2 * h, stacked, 0.0).astype(BF16),
            wo[h * vdim : (h + 1) * vdim, :],
            preferred_element_type=F32,
        )
    attn_out = jnp.sum(spread.reshape(rows, maps, feats), axis=1)
    middle = (tok_ref[...].astype(F32) + attn_out).astype(BF16).astype(F32)
    mid_squares = jnp.sum(middle * middle, axis=1, keepdims=True)
    coarse = mid_squares.astype(BF16).astype(F32)
    fine = mid_squares - coarse
    lane8 = lax.broadcasted_iota(jnp.int32, (rows, 128), 1)
    tail = jnp.where(lane8 < 64, coarse, fine).astype(BF16)
    mixer_in = (middle * mgain_ref[...]).astype(BF16)

    loads[4].wait()

    def up_share(k):
        dst = lax.rem(me + k, n)
        part = jnp.dot(
            mixer_in,
            wu[:, pl.ds(pl.multiple_of(dst * share, share), share)],
            preferred_element_type=F32,
        )
        return part

    def up_step(k):
        u_send[k, :, :share] = up_share(k).astype(BF16)
        u_send[k, :, share:] = tail
        to_peer(4, k, u_send.at[k], u_recv.at[k]).start()

    over_peers(up_step)
    up = up_share(0)
    mixer_squares = mid_squares
    for k in range(1, n):
        to_peer(4, k, u_send.at[k], u_recv.at[k]).wait_recv()
        up += u_recv[k, :, :share].astype(F32)
        ends = u_recv[k, :, share:].astype(F32)
        mixer_squares += ends[:, 0:1] + ends[:, 64:65]
    mixer_inv = lax.rsqrt(mixer_squares / width + EPS)
    lifted = jnp.maximum(mixer_inv * up, 0.0)
    h_all[me] = (lifted * lifted).astype(BF16)
    over_peers(lambda k: to_peer(5, k, h_all.at[me], h_all.at[me]).start())

    loads[5].wait()

    def down_part(src):
        return jnp.dot(
            h_all[src],
            wd[pl.ds(pl.multiple_of(src * share, share), share), :],
            preferred_element_type=F32,
        )

    def down_step(k, so_far):
        src = lax.rem(me + n - k, n)
        to_peer(5, k, h_all.at[me], h_all.at[src]).wait_recv()
        return so_far + down_part(src)

    mixer_out = lax.fori_loop(1, n, down_step, down_part(me))
    out_ref[...] = (middle + mixer_out).astype(BF16)

    def drain(k):
        to_peer(0, k, q_send.at[lax.rem(me + k, n)], q_recv.at[k]).wait_send()
        to_peer(1, k, q_all.at[me], q_all.at[me]).wait_send()
        to_peer(2, k, a_send.at[lax.rem(me + k, n)], a_recv.at[k]).wait_send()
        to_peer(3, k, n_all.at[me], n_all.at[me]).wait_send()
        to_peer(4, k, u_send.at[k], u_recv.at[k]).wait_send()
        to_peer(5, k, h_all.at[me], h_all.at[me]).wait_send()

    over_peers(drain)


def fused(
    n,
    tokens,
    attn_gain,
    query_weight,
    key_cache,
    value_cache,
    lambdas,
    head_gain,
    out_weight,
    mixer_gain,
    up_weight,
    down_weight,
):
    rows, feats = tokens.shape
    _, places, heads, two, hd = key_cache.shape
    vdim = value_cache.shape[3]
    maps = heads * two
    share = up_weight.shape[1] // n
    per = maps * rows // n
    half = hd // 2
    inverse = np.float32(10000.0) ** (-np.arange(half, dtype=np.float32) / np.float32(half))
    angle = np.float32(places * n - 1) * inverse.astype(np.float32)
    cosine = np.cos(angle).astype(np.float32)
    sine = np.sin(angle).astype(np.float32)
    cos_row = np.concatenate([cosine, cosine])[None]
    sin_row = np.concatenate([-sine, sine])[None]
    keys = key_cache.reshape(rows, places * maps, hd)
    values = value_cache.reshape(rows, places * heads, vdim)
    vmem = pl.BlockSpec(memory_space=pltpu.VMEM)
    smem = pl.BlockSpec(memory_space=pltpu.SMEM)
    hbm = pl.BlockSpec(memory_space=pl.ANY)
    return pl.pallas_call(
        functools.partial(layer_kernel, n, feats * n),
        out_shape=jax.ShapeDtypeStruct((rows, feats), BF16),
        in_specs=[vmem, vmem, smem] + [vmem] * 4 + [hbm] * 6,
        out_specs=vmem,
        scratch_shapes=[
            pltpu.VMEM(query_weight.shape, BF16),
            pltpu.VMEM(keys.shape, BF16),
            pltpu.VMEM(values.shape, BF16),
            pltpu.VMEM(out_weight.shape, BF16),
            pltpu.VMEM(up_weight.shape, BF16),
            pltpu.VMEM(down_weight.shape, BF16),
            pltpu.VMEM((n, rows, 2 * hd), F32),
            pltpu.VMEM((n, rows, 2 * hd), F32),
            pltpu.VMEM((n, rows, hd), BF16),
            pltpu.VMEM((n, per, vdim + 128), F32),
            pltpu.VMEM((n, per, vdim + 128), F32),
            pltpu.VMEM((n, per, vdim), BF16),
            pltpu.VMEM((n, rows, share + 128), BF16),
            pltpu.VMEM((n, rows, share + 128), BF16),
            pltpu.VMEM((n, rows, share), BF16),
            pltpu.SemaphoreType.DMA((6,)),
            pltpu.SemaphoreType.DMA((6, n)),
            pltpu.SemaphoreType.DMA((6, n)),
        ],
        compiler_params=pltpu.CompilerParams(
            collective_id=0, has_side_effects=True, vmem_limit_bytes=60 * 1024 * 1024
        ),
    )(
        tokens,
        attn_gain[None],
        lambdas,
        head_gain[None],
        mixer_gain[None],
        jnp.asarray(cos_row),
        jnp.asarray(sin_row),
        query_weight,
        keys,
        values,
        out_weight,
        up_weight,
        down_weight,
    )


def fits(
    n,
    tokens,
    attn_gain,
    query_weight,
    key_cache,
    value_cache,
    lambdas,
    head_gain,
    out_weight,
    mixer_gain,
    up_weight,
    down_weight,
):
    rows, feats = tokens.shape
    _, places, heads, two, hd = key_cache.shape
    maps = heads * two
    return (
        lax.axis_size("tp") == 1
        and n == maps
        and hd == 128
        and rows % 8 == 0
        and maps * rows == 8 * n
        and maps % 8 == 0
        and feats % 128 == 0
        and (places * maps) % 256 == 0
        and up_weight.shape[1] % (128 * n) == 0
    )


def layer(*args):
    n = lax.axis_size("kv")
    return fused(n, *args) if fits(n, *args) else local(*args)


def solution(mesh):
    return jax.shard_map(
        layer,
        mesh=mesh,
        in_specs=(
            P("dp", "kv"),
            P("kv"),
            P("kv", "tp"),
            P("dp", "kv", "tp", None, None),
            P("dp", "kv", "tp", None),
            P("tp"),
            P(),
            P("tp", "kv"),
            P("kv"),
            P("kv", "tp"),
            P("tp", "kv"),
        ),
        out_specs=P("dp", "kv"),
        check_vma=False,
    )
```
